128 devices in a mesh: sp: 32 (over z, y, core), tp: 4 (over x).
Axes of the slice: x: 4, y: 4, z: 4, core: 2. Of those that a mesh axis runs over, the one named last changes fastest.
Arguments:
- residual_in: bfloat16 [16384, 2048], P('sp'), may hold values from -6 to 6
- queries_nope: bfloat16 [16384, 1024], P('sp', 'tp'), may hold values from -15 to 15
- queries_rope: bfloat16 [16384, 512], P('sp', 'tp'), may hold values from -400 to 400
- latents: bfloat16 [16384, 256], P('sp'), may hold values from -6 to 6
- rope_keys: bfloat16 [16384, 32], P('sp'), may hold values from -8 to 8
- latent_norm_gain: float32 [256], replicated, may hold values from 0.1 to 1.9
- key_up_weight: bfloat16 [256, 1024], P(None, 'tp'), may hold values from -0.375 to 0.375
- value_up_weight: bfloat16 [256, 1024], P(None, 'tp'), may hold values from -0.375 to 0.375
- w_out: bfloat16 [1024, 2048], P('tp'), may hold values from -0.59765625 to 0.59765625
- norm_gain: float32 [2048], replicated, may hold values from 0.1 to 1.9
- w_up: bfloat16 [2048, 8192], P('sp', 'tp'), may hold values from -0.125 to 0.125
- w_down: bfloat16 [8192, 2048], P('tp', 'sp'), may hold values from -0.0625 to 0.0625
Outputs:
- layer_out: bfloat16 [16384, 2048], P('sp', 'tp')
The draws below stay inside these ranges and needn't reach their ends.
All inputs are finite; a program needn't handle non-finite values.
Results may differ from the reference program's by a relative error of at most 0.015.
Values may be sent and summed in bfloat16 or wider, within the bound.
No kernel may reach another device: no remote copies, remote signals or barrier semaphores. Data moves between devices by JAX's collectives and lax.ppermute only.
A program may use at most 128 MiB of HBM per device.

```python
import math
import jax
import jax.numpy as jnp
from jax import lax

D = 2048
HEAD_TOTAL = 16
UNROTATED_WIDTH = 64
ROPE = 32
VALUE_WIDTH = 64
LATENT_WIDTH = 256
FF = 8192
TOKEN_TOTAL = 16384
N_TP = 4


def shared_rope(key):
    base_rows = jnp.clip(jax.random.normal(jax.random.fold_in(key, 11), (TOKEN_TOTAL, ROPE), jnp.float32), -4.0, 4.0)
    return base_rows


def draw_rope_keys(key, part):
    base_rows = shared_rope(key)
    return base_rows.astype(jnp.bfloat16)


def draw_queries_rope(key, part):
    drawn = jnp.clip(jax.random.normal(jax.random.fold_in(key, 21), (TOKEN_TOTAL, HEAD_TOTAL * ROPE), jnp.float32) * 2.5, -15.0, 15.0)
    return drawn.astype(jnp.bfloat16)


def level_of(stream_key, dims, shards, least, largest):
    factor_of, own = 1.0, jax.random.fold_in(stream_key, 6)
    for axis_at, blocks in shards:
        draws = jnp.exp(jax.random.uniform(jax.random.fold_in(own, axis_at), (blocks,), jnp.float32, least / len(shards), largest / len(shards)))
        factor_of = factor_of * jnp.repeat(draws, dims[axis_at] // blocks).reshape([-1 if axis == axis_at else 1 for axis in range(len(dims))])
    return factor_of


def bell_draw(own_key, extent, scale, reach, pieces=(), kind=jnp.bfloat16):
    gain = level_of(own_key, extent, pieces, -0.22, 0.18) if pieces else 1.0
    entries = jax.random.normal(own_key, extent, jnp.float32) * scale * gain
    return jnp.minimum(jnp.maximum(entries, -reach), reach).astype(kind)


def setup_inputs(seed: int = 0) -> dict:
    keys = jax.random.split(jax.random.key(seed), 13)
    residual_in = bell_draw(keys[0], (TOKEN_TOTAL, D), 1.0, 6.0, ((0, 32),))
    queries_nope = bell_draw(keys[1], (TOKEN_TOTAL, HEAD_TOTAL * UNROTATED_WIDTH), 2.5, 15.0, ((0, 32), (1, 4)))
    queries_rope = draw_queries_rope(jax.random.fold_in(keys[12], 71), 0)
    latents = bell_draw(keys[3], (TOKEN_TOTAL, LATENT_WIDTH), 1.0, 6.0, ((0, 32),))
    rope_keys = draw_rope_keys(jax.random.fold_in(keys[12], 71), 0)
    latent_norm_gain = jnp.clip(1.0 + 0.18 * jax.random.normal(keys[5], (LATENT_WIDTH,), jnp.float32), 0.1, 1.9)
    key_up_weight = bell_draw(keys[6], (LATENT_WIDTH, HEAD_TOTAL * UNROTATED_WIDTH), LATENT_WIDTH ** -0.5, 0.375, ((1, 4),))
    value_up_weight = bell_draw(keys[7], (LATENT_WIDTH, HEAD_TOTAL * VALUE_WIDTH), LATENT_WIDTH ** -0.5, 0.375, ((1, 4),))
    w_out = bell_draw(keys[8], (HEAD_TOTAL * VALUE_WIDTH, D), 0.1, 0.59765625, ((0, 4),))
    norm_gain = jnp.clip(1.0 + 0.18 * jax.random.normal(keys[9], (D,), jnp.float32), 0.1, 1.9)
    w_up = bell_draw(keys[10], (D, FF), D ** -0.5, 0.125, ((0, 32), (1, 4)))
    w_down = bell_draw(keys[11], (FF, D), FF ** -0.5, 0.0625, ((0, 4), (1, 32)))
    return dict(residual_in=residual_in, queries_nope=queries_nope, queries_rope=queries_rope, latents=latents, rope_keys=rope_keys, latent_norm_gain=latent_norm_gain, key_up_weight=key_up_weight, value_up_weight=value_up_weight, w_out=w_out, norm_gain=norm_gain, w_up=w_up, w_down=w_down)


rope_base = 10000.0
epsilon = 1e-06

def rotate(vectors, phases):
    half_width = vectors.shape[-1] // 2
    first_half = vectors[..., :half_width]
    second_half = vectors[..., half_width:]
    cosine = jnp.cos(phases)
    sine = jnp.sin(phases)
    return jnp.concatenate([first_half * cosine - second_half * sine, second_half * cosine + first_half * sine], axis=-1)

def rope_phases(positions, width):
    inverse = 1.0 / rope_base ** (jnp.arange(0, width, 2, dtype=jnp.float32) / width)
    return positions.astype(jnp.float32)[:, None] * inverse[None, :]

def rms_scale(vectors, gain_vec):
    return vectors * lax.rsqrt(lax.optimization_barrier(jnp.mean(vectors * vectors, axis=-1, keepdims=True)) + epsilon) * gain_vec.astype(jnp.float32)

def reference(residual_in, queries_nope, queries_rope, latents, rope_keys, latent_norm_gain, key_up_weight, value_up_weight, w_out, norm_gain, w_up, w_down):
    positions = jnp.arange(TOKEN_TOTAL, dtype=jnp.int32)
    phases = rope_phases(positions, ROPE)
    q_rot = rotate(queries_rope.astype(jnp.float32).reshape(TOKEN_TOTAL, HEAD_TOTAL, ROPE), phases[:, None, :]).astype(jnp.bfloat16)
    queries = jnp.concatenate([queries_nope.reshape(TOKEN_TOTAL, HEAD_TOTAL, UNROTATED_WIDTH), q_rot], axis=2)
    lat_norm = rms_scale(latents.astype(jnp.float32), latent_norm_gain).astype(jnp.bfloat16)
    key_nope = jnp.dot(lat_norm, key_up_weight, preferred_element_type=jnp.float32).astype(jnp.bfloat16).reshape(TOKEN_TOTAL, HEAD_TOTAL, UNROTATED_WIDTH)
    values = jnp.dot(lat_norm, value_up_weight, preferred_element_type=jnp.float32).astype(jnp.bfloat16).reshape(TOKEN_TOTAL, HEAD_TOTAL, VALUE_WIDTH)
    key_rot = rotate(rope_keys.astype(jnp.float32), phases).astype(jnp.bfloat16)
    key_all = jnp.concatenate([key_nope, jnp.broadcast_to(key_rot[:, None, :], (TOKEN_TOTAL, HEAD_TOTAL, ROPE))], axis=2).astype(jnp.float32)
    value_all = values.astype(jnp.float32)
    score_scale = 1.0 / math.sqrt(UNROTATED_WIDTH + ROPE)
    query_rows = math.gcd(TOKEN_TOTAL, 128)

    def attend(query_block):
        scores = jnp.einsum('qhd,khd->hqk', query_block.astype(jnp.float32), key_all) * score_scale
        row_peak = lax.optimization_barrier(jnp.max(scores, axis=2, keepdims=True))
        weights = jnp.exp(scores - row_peak)
        denominator = lax.optimization_barrier(jnp.sum(weights, axis=2))
        rounded = lax.optimization_barrier(weights.astype(jnp.bfloat16)).astype(jnp.float32)
        weighted = jnp.einsum('hqk,khd->qhd', rounded, value_all)
        return (weighted / jnp.transpose(denominator)[:, :, None]).astype(jnp.bfloat16)
    attended = lax.map(attend, queries.reshape(TOKEN_TOTAL // query_rows, query_rows, HEAD_TOTAL, UNROTATED_WIDTH + ROPE))
    attended = attended.reshape(TOKEN_TOTAL, HEAD_TOTAL * VALUE_WIDTH)
    group_cols = HEAD_TOTAL * VALUE_WIDTH // N_TP
    summed = jnp.zeros((TOKEN_TOTAL, D), jnp.float32)
    for member in range(N_TP):
        part_term = jnp.dot(attended[:, member * group_cols:(member + 1) * group_cols], w_out[member * group_cols:(member + 1) * group_cols], preferred_element_type=jnp.float32)
        summed = summed + lax.optimization_barrier(part_term.astype(jnp.bfloat16)).astype(jnp.float32)
    stream = residual_in.astype(jnp.float32) + summed
    normed = rms_scale(stream, norm_gain).astype(jnp.bfloat16)
    upward = jnp.dot(normed, w_up, preferred_element_type=jnp.float32)
    hidden = jnp.square(jax.nn.relu(upward)).astype(jnp.bfloat16)
    group_units = FF // N_TP
    mixer = jnp.zeros((TOKEN_TOTAL, D), jnp.float32)
    for member in range(N_TP):
        part_term = jnp.dot(hidden[:, member * group_units:(member + 1) * group_units], w_down[member * group_units:(member + 1) * group_units], preferred_element_type=jnp.float32)
        mixer = mixer + lax.optimization_barrier(part_term.astype(jnp.bfloat16)).astype(jnp.float32)
    return (stream + mixer).astype(jnp.bfloat16)
```

```python
import functools
import math

import jax
import jax.numpy as jnp
from jax import lax
from jax.experimental import pallas as pl
from jax.experimental.pallas import tpu as pltpu
from jax.sharding import PartitionSpec as P

UNROTATED_WIDTH = 64
ROPE = 32
VALUE_WIDTH = 64
LANES = 128
ROPE_END = UNROTATED_WIDTH + ROPE
VALUE_ROWS = 80
HEADROOM = 8.0
SUBBLOCKS = 4

rope_base = 10000.0
epsilon = 1e-06
SCALE = math.log2(math.e) / math.sqrt(ROPE_END)


def rotate(vectors, phases):
    half_width = vectors.shape[-1] // 2
    first_half = vectors[..., :half_width]
    second_half = vectors[..., half_width:]
    cosine = jnp.cos(phases)
    sine = jnp.sin(phases)
    return jnp.concatenate(
        [first_half * cosine - second_half * sine, second_half * cosine + first_half * sine],
        axis=-1,
    )


def rope_phases(positions, width):
    inverse = 1.0 / rope_base ** (jnp.arange(0, width, 2, dtype=jnp.float32) / width)
    return positions.astype(jnp.float32)[:, None] * inverse[None, :]


def rms_scale(vectors, gain_vec):
    return (
        vectors
        * lax.rsqrt(jnp.mean(vectors * vectors, axis=-1, keepdims=True) + epsilon)
        * gain_vec
    )


def dot(a, b, dims):
    return lax.dot_general(a, b, (dims, ((), ())), preferred_element_type=jnp.float32)


def attention_kernel(
    tokens,
    packed,
    latent_ref,
    key_up_ref,
    value_up_ref,
    query_ref,
    out_ref,
    shifted_ref,
    offset_ref,
    total_ref,
    block_ref,
    key_ref,
    value_ref,
):
    step = pl.program_id(0)
    heads, _, rows = query_ref.shape
    pieces = latent_ref.shape[0]
    groups = latent_ref.shape[2] // ROPE
    per_tile = LANES // ROPE

    @pl.when(step == 0)
    def _():
        shifted_ref[...] = query_ref[...]
        offset_ref[...] = jnp.zeros_like(offset_ref)
        total_ref[...] = jnp.zeros_like(total_ref)
        ones = lax.broadcasted_iota(
            jnp.int32, (heads, VALUE_ROWS - VALUE_WIDTH, value_ref.shape[2]), 1
        )
        value_ref[:, VALUE_WIDTH:, :] = jnp.where(ones == 0, 1.0, 0.0).astype(jnp.bfloat16)

    lane = lax.broadcasted_iota(jnp.int32, (packed, LANES), 1)
    is_rope = (lane >= UNROTATED_WIDTH) & (lane < ROPE_END)
    fill = jnp.where((lane == ROPE_END) | (lane == ROPE_END + 1), 1.0, 0.0)
    for piece in range(pieces):
        latent = latent_ref[piece, :tokens, :]
        keys = dot(latent, key_up_ref[...], ((1,), (0,)))
        for group in range(groups):
            tile = group // per_tile
            turned = latent_ref[piece, tokens:, tile * LANES : (tile + 1) * LANES]
            turned = turned.astype(jnp.float32)
            shift = (UNROTATED_WIDTH - ROPE * (group % per_tile)) % LANES
            if shift:
                turned = pltpu.roll(turned, shift, 1)
            turned = jnp.where(is_rope, turned, fill)
            for head in range(heads):
                own = keys[group * packed : (group + 1) * packed, head * LANES : (head + 1) * LANES]
                begin = piece * tokens + group * packed
                key_ref[head, begin : begin + packed, :] = (own * SCALE + turned).astype(
                    jnp.bfloat16
                )
        values = dot(value_up_ref[...], latent, ((1,), (1,))).astype(jnp.bfloat16)
        for head in range(heads):
            value_ref[head, :VALUE_WIDTH, piece * tokens : (piece + 1) * tokens] = values[
                head * VALUE_WIDTH : (head + 1) * VALUE_WIDTH, :
            ]

    peaks = []
    for head in range(heads):
        scores = dot(key_ref[head], shifted_ref[head], ((1,), (0,)))
        peaks.append(jnp.max(scores, axis=0, keepdims=True))
        weights = jnp.exp2(scores).astype(jnp.bfloat16)
        block_ref[head] = dot(value_ref[head], weights, ((1,), (0,)))
    peak = functools.reduce(jnp.maximum, peaks)
    rescale = (jnp.max(peak) > HEADROOM) | (step == 0)

    @pl.when(jnp.logical_not(rescale))
    def _():
        for head in range(heads):
            total_ref[head] = total_ref[head] + block_ref[head]

    @pl.when(rescale)
    def _():
        def one_head(head, carry):
            scores = dot(key_ref[head], shifted_ref[head], ((1,), (0,)))
            rise = jnp.max(scores, axis=0, keepdims=True)
            rise = jnp.where(step == 0, rise, jnp.maximum(rise, 0.0))
            old = offset_ref[head, 0:1, :]
            wanted = old + rise
            high = wanted.astype(jnp.bfloat16).astype(jnp.float32)
            low = (wanted - high).astype(jnp.bfloat16).astype(jnp.float32)
            new = high + low
            offset_ref[head, 0:1, :] = new
            row = lax.broadcasted_iota(jnp.int32, (16, rows), 0)
            shifted_ref[head, ROPE_END : ROPE_END + 16, :] = jnp.where(
                row == 0, -high, jnp.where(row == 1, -low, 0.0)
            ).astype(jnp.bfloat16)
            scores = dot(key_ref[head], shifted_ref[head], ((1,), (0,)))
            weights = jnp.exp2(scores).astype(jnp.bfloat16)
            factor = jnp.where(step == 0, 0.0, jnp.exp2(jnp.minimum(old - new, 0.0)))
            total_ref[head] = total_ref[head] * factor + dot(
                value_ref[head], weights, ((1,), (0,))
            )
            return carry

        lax.fori_loop(0, heads, one_head, 0)

    @pl.when(step == pl.num_programs(0) - 1)
    def _():
        for head in range(heads):
            total = total_ref[head]
            out_ref[head * VALUE_WIDTH : (head + 1) * VALUE_WIDTH, :] = (
                total[:VALUE_WIDTH] / total[VALUE_WIDTH : VALUE_WIDTH + 1]
            ).astype(jnp.bfloat16)


def attend(gathered, key_up, value_up, queries, tokens):
    devices, height, width = gathered.shape
    heads, _, rows = queries.shape
    pieces = math.gcd(devices, SUBBLOCKS)
    block = pieces * tokens
    return pl.pallas_call(
        functools.partial(attention_kernel, tokens, height - tokens),
        grid=(devices // pieces,),
        in_specs=[
            pl.BlockSpec((pieces, height, width), lambda i: (i, 0, 0)),
            pl.BlockSpec(key_up.shape, lambda i: (0, 0)),
            pl.BlockSpec(value_up.shape, lambda i: (0, 0)),
            pl.BlockSpec(queries.shape, lambda i: (0, 0, 0)),
        ],
        out_specs=pl.BlockSpec((heads * VALUE_WIDTH, rows), lambda i: (0, 0)),
        out_shape=jax.ShapeDtypeStruct((heads * VALUE_WIDTH, rows), jnp.bfloat16),
        scratch_shapes=[
            pltpu.VMEM(queries.shape, jnp.bfloat16),
            pltpu.VMEM((heads, 8, rows), jnp.float32),
            pltpu.VMEM((heads, VALUE_ROWS, rows), jnp.float32),
            pltpu.VMEM((heads, VALUE_ROWS, rows), jnp.float32),
            pltpu.VMEM((heads, block, LANES), jnp.bfloat16),
            pltpu.VMEM((heads, VALUE_ROWS, block), jnp.bfloat16),
        ],
        compiler_params=pltpu.CompilerParams(
            dimension_semantics=("arbitrary",), vmem_limit_bytes=50 * 1024 * 1024
        ),
        cost_estimate=pl.CostEstimate(
            flops=2 * heads * rows * devices * tokens * (LANES + VALUE_ROWS),
            bytes_accessed=gathered.size * 2,
            transcendentals=heads * rows * devices * tokens,
        ),
        name="attention",
    )(gathered, key_up, value_up, queries)


def in_blocks(x, dim, count):
    dims = x.shape
    parts = x.reshape(*dims[:dim], count, dims[dim] // count, *dims[dim + 1 :])
    return jnp.moveaxis(parts, dim, 0)


def sent_and_summed(x, axis, dim):
    count = lax.axis_size(axis)
    parts = lax.all_to_all(in_blocks(x, dim, count), axis, 0, 0, tiled=True)
    return jnp.sum(parts.astype(jnp.float32), axis=0)


def from_others(x, axis):
    count = lax.axis_size(axis)
    shifts = sorted(range(1, count), key=lambda k: -min(k, count - k))
    return {0: x} | {
        k: lax.ppermute(x, axis, [(i, (i + k) % count) for i in range(count)]) for k in shifts
    }


def on_device(
    residual_in,
    queries_nope,
    queries_rope,
    latents,
    rope_keys,
    latent_norm_gain,
    key_up_weight,
    value_up_weight,
    w_out,
    norm_gain,
    w_up,
    w_down,
):
    rows = residual_in.shape[0]
    heads = key_up_weight.shape[1] // UNROTATED_WIDTH
    latent_width = latents.shape[1]
    positions = lax.axis_index("sp") * rows + jnp.arange(rows, dtype=jnp.int32)
    phases = rope_phases(positions, ROPE)
    lat_norm = rms_scale(latents.astype(jnp.float32), latent_norm_gain).astype(jnp.bfloat16)
    key_rot = (rotate(rope_keys.astype(jnp.float32), phases) * SCALE).astype(jnp.bfloat16)
    groups = latent_width // ROPE
    packed = rows // groups
    key_rot = jnp.moveaxis(key_rot.reshape(groups, packed, ROPE), 0, 1)
    sent = jnp.concatenate([lat_norm, key_rot.reshape(packed, latent_width)], axis=0)
    gathered = lax.all_gather(sent, "sp", axis=0, tiled=False)

    whole_up = lax.all_gather(w_up, "sp", axis=0, tiled=True)
    whole_down = lax.all_gather(w_down, "sp", axis=1, tiled=True)
    out_parts = from_others(w_out, "tp")

    q_rot = rotate(
        queries_rope.astype(jnp.float32).reshape(rows, heads, ROPE), phases[:, None, :]
    ).astype(jnp.bfloat16)
    queries = jnp.concatenate(
        [
            queries_nope.reshape(rows, heads, UNROTATED_WIDTH),
            q_rot,
            jnp.zeros((rows, heads, LANES - ROPE_END), jnp.bfloat16),
        ],
        axis=2,
    )
    queries = jnp.transpose(queries, (1, 2, 0))
    key_up = jnp.pad(
        key_up_weight.reshape(latent_width, heads, UNROTATED_WIDTH),
        ((0, 0), (0, 0), (0, LANES - UNROTATED_WIDTH)),
    ).reshape(latent_width, heads * LANES)
    attended = attend(gathered, key_up, value_up_weight.T, queries, rows)

    parts = from_others(attended, "tp")
    stream = residual_in.astype(jnp.float32)
    for k in parts:
        stream = stream + dot(parts[k], out_parts[k], ((0,), (0,)))
    normed = rms_scale(stream, norm_gain).astype(jnp.bfloat16)
    upward = jnp.dot(normed, whole_up, preferred_element_type=jnp.float32)
    hidden = jnp.square(jax.nn.relu(upward)).astype(jnp.bfloat16)
    terms = jnp.dot(hidden, whole_down, preferred_element_type=jnp.float32)
    mixer = sent_and_summed(terms.astype(jnp.bfloat16), "tp", 1)
    own_width = mixer.shape[1]
    own_stream = lax.dynamic_slice_in_dim(stream, lax.axis_index("tp") * own_width, own_width, 1)
    return (own_stream + mixer).astype(jnp.bfloat16)


def solution(mesh):
    in_specs = (
        P("sp", None),
        P("sp", "tp"),
        P("sp", "tp"),
        P("sp", None),
        P("sp", None),
        P(),
        P(None, "tp"),
        P(None, "tp"),
        P("tp", None),
        P(),
        P("sp", "tp"),
        P("tp", "sp"),
    )
    out_specs = P("sp", "tp")
    return jax.shard_map(
        on_device, mesh=mesh, in_specs=in_specs, out_specs=out_specs, check_vma=False
    )
```
